32 devices in a mesh: grp: 2 (over y), dp: 2 (over x), kv: 4 (over z), tp: 2 (over core).
Axes of the slice: x: 2, y: 2, z: 4, core: 2. Of those that a mesh axis runs over, the one named last changes fastest.
Arguments:
- tokens: bfloat16 [32, 2048], P(('grp', 'dp'), ('kv', 'tp')), parts along dimension 0, may hold values from -40 to 40
- past_state: float32 [32, 16, 128, 128], P(('grp', 'dp', 'kv'), 'tp'), parts along dimension 0, may hold values from -4 to 4
- mix_gain: float32 [2048], P('kv'), may hold values from 0.1 to 1.9
- w_query: bfloat16 [2048, 2048], P('kv', 'tp'), may hold values from -0.125 to 0.125
- w_forget: bfloat16 [2048, 2048], P('kv', 'tp'), may hold values from -0.125 to 0.125
- w_value: bfloat16 [2048, 2048], P('kv', 'tp'), may hold values from -0.125 to 0.125
- w_gate_out: bfloat16 [2048, 2048], P('kv', 'tp'), may hold values from -0.125 to 0.125
- floor_logits: float32 [2048], P('tp'), may hold values from -6 to 6
- head_gain: float32 [128], replicated, may hold values from 0.1 to 1.9
- w_out: bfloat16 [2048, 2048], P(None, ('kv', 'tp')), may hold values from -0.125 to 0.125
- mlp_gain: float32 [2048], replicated, may hold values from 0.1 to 1.9
- w_gate: bfloat16 [2048, 5632], P(None, ('kv', 'tp')), may hold values from -0.125 to 0.125
- w_up: bfloat16 [2048, 5632], P(None, ('kv', 'tp')), may hold values from -0.125 to 0.125
- w_down: bfloat16 [5632, 2048], P(('kv', 'tp')), may hold values from -0.109375 to 0.109375
Outputs:
- result: bfloat16 [32, 2048], P(('grp', 'dp'), ('kv', 'tp')), parts along dimension 0
- new_state: float32 [32, 16, 128, 128], P(('grp', 'dp', 'kv'), 'tp'), parts along dimension 0
The draws below stay inside these ranges and needn't reach their ends.
There are 2 independent parts, one for each index of `grp`. The reference program is written for one: setup_inputs(seed, part) draws one part's arguments, and reference() takes and returns one part's arrays. A program takes and returns all parts, laid end to end along the dimension named above; an argument that names none is the same for every part. Nothing has to cross between parts.
All inputs are finite; a program needn't handle non-finite values.
Results may differ from the reference program's by a relative error of at most 0.0091.
Values may be sent and summed in bfloat16 or wider, within the bound.
A program may use at most 64 MiB of HBM per device.

```python
import math
import jax
import jax.numpy as jnp
from jax import lax

D = 2048
H = 16
DK = 128
DV = 128
FF = 5632
HK = 2048
HV = 2048
SEQS = 16


def draw_tokens(key, part):
    key_base = jax.random.fold_in(key, 101)
    key_rows = jax.random.fold_in(key, 202)
    columns = 10.0 ** (0.5 * (jnp.arange(D, dtype=jnp.float32) / D - 0.5))
    rows = jnp.exp(jax.random.uniform(key_rows, (SEQS, 1), jnp.float32, math.log(0.3), math.log(3.0)))
    base = jnp.clip(jax.random.normal(key_base, (SEQS, D), jnp.float32), -6.0, 6.0)
    return (base * columns * rows).astype(jnp.bfloat16)


def strengthened(drawn, key, source, target, blocks, factor):
    def block_of(position):
        return (jnp.arange(drawn.shape[position]) // (drawn.shape[position] // blocks)).reshape((-1,) + (1,) * (drawn.ndim - 1 - position))

    first = jax.random.permutation(key, blocks)[block_of(target)]
    far = (block_of(target) + blocks // 2) % blocks
    return jnp.where((block_of(source) == first) | (block_of(source) == far), factor * drawn, drawn)


def block_levels(stream_key, shape, split, least, largest):
    factor_of, own = 1.0, jax.random.fold_in(stream_key, 6)
    for position, parts in split:
        draws = jnp.exp(jax.random.uniform(jax.random.fold_in(own, position), (parts,), jnp.float32, least / len(split), largest / len(split)))
        factor_of = factor_of * jnp.repeat(draws, shape[position] // parts).reshape([-1 if axis == position else 1 for axis in range(len(shape))])
    return factor_of


def bell_draw(own_key, extent, deviation, limit, pieces=(), kind=jnp.bfloat16):
    values = jax.random.normal(own_key, extent, jnp.float32) * deviation
    if len(pieces) > 0:
        values = block_levels(own_key, extent, pieces, -0.22, 0.18) * values
    return jnp.clip(values, min=-limit, max=limit).astype(kind)


def bell_draw_with(rng, shape, spread, bound, shards, heavy, held_as=jnp.bfloat16):
    array = spread * jax.random.normal(rng, shape, jnp.float32)
    if shards:
        array = array * block_levels(rng, shape, shards, -0.22, 0.18)
    return jnp.clip(strengthened(array, jax.random.fold_in(rng, 3), *heavy), -bound, bound).astype(held_as)


def setup_inputs(seed: int = 0, part: int = 0) -> dict:
    keys = jax.random.split(jax.random.key(seed), 15)
    own_keys = jax.random.split(jax.random.fold_in(keys[14], part), 15)
    tokens = draw_tokens(jax.random.fold_in(jax.random.fold_in(keys[14], part), 71), part)
    past_state = bell_draw(own_keys[1], (SEQS, H, DK, DV), 0.5, 4.0, ((0, 8), (1, 2)), jnp.float32)
    mix_gain = jnp.clip(1.0 + 0.18 * jax.random.normal(keys[2], (D,), jnp.float32), 0.1, 1.9)
    w_query = bell_draw(keys[3], (D, HK), D ** -0.5, 0.125, ((0, 4), (1, 2)))
    w_forget = bell_draw(keys[4], (D, HK), D ** -0.5, 0.125, ((0, 4), (1, 2)))
    w_value = bell_draw(keys[5], (D, HV), D ** -0.5, 0.125, ((0, 4), (1, 2)))
    w_gate_out = bell_draw(keys[6], (D, HV), D ** -0.5, 0.125, ((0, 4), (1, 2)))
    floor_logits = bell_draw(keys[7], (HK,), 1.5, 6.0, ((0, 2),), jnp.float32)
    head_gain = jnp.clip(1.0 + 0.18 * jax.random.normal(keys[8], (DV,), jnp.float32), 0.1, 1.9)
    w_out = bell_draw(keys[9], (HV, D), HV ** -0.5, 0.125, ((1, 8),))
    mlp_gain = jnp.clip(1.0 + 0.18 * jax.random.normal(keys[10], (D,), jnp.float32), 0.1, 1.9)
    w_gate = bell_draw(keys[11], (D, FF), D ** -0.5, 0.125, ((1, 8),))
    w_up = bell_draw(keys[12], (D, FF), D ** -0.5, 0.125, ((1, 8),))
    w_down = bell_draw_with(keys[13], (FF, D), FF ** -0.5, 0.109375, ((0, 8),), (0, 1, 8, 2.0))
    return dict(tokens=tokens, past_state=past_state, mix_gain=mix_gain, w_query=w_query, w_forget=w_forget, w_value=w_value, w_gate_out=w_gate_out, floor_logits=floor_logits, head_gain=head_gain, w_out=w_out, mlp_gain=mlp_gain, w_gate=w_gate, w_up=w_up, w_down=w_down)


epsilon = 1e-06

def reference(tokens, past_state, mix_gain, w_query, w_forget, w_value, w_gate_out, floor_logits, head_gain, w_out, mlp_gain, w_gate, w_up, w_down):
    count = tokens.shape[0]
    token_f = tokens.astype(jnp.float32)
    row_scale = lax.rsqrt(lax.optimization_barrier(jnp.mean(token_f * token_f, axis=1, keepdims=True)) + epsilon)
    gained = (token_f * mix_gain).astype(jnp.bfloat16)
    query = jnp.dot(gained, w_query, preferred_element_type=jnp.float32) * row_scale
    forget_pre = jnp.dot(gained, w_forget, preferred_element_type=jnp.float32) * row_scale
    value = jnp.dot(gained, w_value, preferred_element_type=jnp.float32) * row_scale
    gate_pre = jnp.dot(gained, w_gate_out, preferred_element_type=jnp.float32) * row_scale
    lower = jax.nn.sigmoid(floor_logits).reshape(H, DK)
    forget = lower + (1.0 - lower) * jax.nn.sigmoid(forget_pre.reshape(count, H, DK))
    values = value.reshape(count, H, DV)
    new_state = forget[..., None] * past_state + (1.0 - forget)[..., None] * values[:, :, None, :]
    activ = jax.nn.silu(query.reshape(count, H, DK))
    head_out = jnp.einsum('shkv,shk->shv', new_state, activ, precision=lax.Precision.HIGHEST)
    normed = head_out * lax.rsqrt(lax.optimization_barrier(jnp.mean(head_out * head_out, axis=2, keepdims=True)) + epsilon)
    normed = normed * head_gain * jax.nn.silu(gate_pre.reshape(count, H, DV))
    mixed = normed.reshape(count, H * DV).astype(jnp.bfloat16)
    middle = (token_f + jnp.dot(mixed, w_out, preferred_element_type=jnp.float32)).astype(jnp.bfloat16)
    middle_f = middle.astype(jnp.float32)
    mlp_scale = lax.rsqrt(lax.optimization_barrier(jnp.mean(middle_f * middle_f, axis=1, keepdims=True)) + epsilon)
    mlp_in = (middle_f * mlp_scale * mlp_gain).astype(jnp.bfloat16)
    gate = jnp.dot(mlp_in, w_gate, preferred_element_type=jnp.float32)
    upward = jnp.dot(mlp_in, w_up, preferred_element_type=jnp.float32)
    hidden = (jax.nn.silu(gate) * upward).astype(jnp.bfloat16)
    result = (middle_f + jnp.dot(hidden, w_down, preferred_element_type=jnp.float32)).astype(jnp.bfloat16)
    return (result, new_state)
```

```python
import functools

import jax
import jax.numpy as jnp
from jax import lax
from jax.experimental import pallas as pl
from jax.experimental.pallas import tpu as pltpu
from jax.sharding import PartitionSpec as P

epsilon = 1e-06
F32 = jnp.float32
BF16 = jnp.bfloat16
MESH = pl.DeviceIdType.MESH


def sigmoid(a):
    return 1.0 / (1.0 + jnp.exp(-a))


def silu(a):
    return a / (1.0 + jnp.exp(-a))


def dot_t(a, b):
    return lax.dot_general(a, b, (((1,), (1,)), ((), ())), preferred_element_type=F32)


def kernel(
    K,
    T,
    tokens,
    past,
    mix_gain,
    w_query,
    w_forget,
    w_value,
    w_gate_out,
    floor_logits,
    head_gain,
    w_out,
    mlp_gain,
    w_gate,
    w_up,
    w_down,
    result,
    new_state,
    tok_v,
    past_v,
    mixg_v,
    proj_v,
    floor_v,
    hgain_v,
    wout_v,
    mlpg_v,
    wgate_v,
    wup_v,
    wdown_v,
    new_v,
    sq_send,
    sq_recv,
    part,
    part_send,
    part_recv,
    head_v,
    mix_all,
    mix_f,
    mid_all,
    term_send,
    term_recv,
    res_v,
    local_sem,
    tok_ss,
    tok_rs,
    sq_ss,
    sq_rs,
    part_ss,
    part_rs,
    mix_ss,
    mix_rs,
    mid_ss,
    mid_rs,
    term_ss,
    term_rs,
):
    R, W = tokens.shape
    RL, H, DK, DV = past.shape
    D = w_gate.shape[1]
    kv = lax.axis_index("kv")
    tp = lax.axis_index("tp")
    me = kv * T + tp

    def far(k):
        return min(k, K - k)

    hops = sorted(range(1, K), key=far)
    near = [(0, dt) for dt in range(1, T)] + [(dk, dt) for dk in hops for dt in range(T)]

    def other(dk, dt):
        return lax.rem(kv + dk, K), lax.rem(tp + dt, T)

    def source(dk, dt):
        return lax.rem(kv + K - dk, K), lax.rem(tp + T - dt, T)

    def load(i, src, dst):
        copy = pltpu.make_async_copy(src, dst, local_sem.at[i])
        copy.start()
        return copy

    c_tok = load(0, tokens, tok_v.at[tp])
    c_mixg = load(1, mix_gain, mixg_v)
    c_proj = [
        load(2 + i, w, proj_v.at[i])
        for i, w in enumerate((w_forget, w_query, w_value, w_gate_out))
    ]
    c_past = load(6, past, past_v)
    c_floor = load(7, floor_logits, floor_v)
    c_hgain = load(8, head_gain, hgain_v)
    c_mlpg = load(9, mlp_gain, mlpg_v)
    c_wout = load(10, w_out, wout_v)
    c_wgate = load(11, w_gate, wgate_v)
    c_wup = load(12, w_up, wup_v)
    c_wdown = load(13, w_down, wdown_v)

    barrier = pltpu.get_barrier_semaphore()
    for dk, dt in near:
        k, t = other(dk, dt)
        pl.semaphore_signal(barrier, inc=1, device_id={"kv": k, "tp": t}, device_id_type=MESH)
    c_tok.wait()
    pl.semaphore_wait(barrier, len(near))

    def send(src, dst, ss, rs, k, t):
        copy = pltpu.make_async_remote_copy(
            src_ref=src,
            dst_ref=dst,
            send_sem=ss,
            recv_sem=rs,
            device_id={"kv": k, "tp": t},
            device_id_type=MESH,
        )
        copy.start()
        return copy

    def arrived(dst, ss, rs):
        pltpu.make_async_remote_copy(
            src_ref=dst,
            dst_ref=dst,
            send_sem=ss,
            recv_sem=rs,
            device_id={"kv": kv, "tp": lax.rem(tp + 1, T)},
            device_id_type=MESH,
        ).wait_recv()

    sent = []
    for dt in range(1, T):
        k, t = other(0, dt)
        sent.append(send(tok_v.at[tp], tok_v.at[tp], tok_ss.at[dt], tok_rs.at[tp], k, t))

    c_mixg.wait()
    gained = []
    square = jnp.zeros((R, 1), F32)
    for dt in range(T):
        t = lax.rem(tp + T - dt, T)
        if dt:
            arrived(tok_v.at[t], tok_ss.at[0], tok_rs.at[t])
        block = tok_v[t].astype(F32)
        square = square + jnp.sum(block * block, axis=1, keepdims=True)
        gained.append((block * mixg_v[t]).astype(BF16))
    square = jnp.broadcast_to(square, (R, DK))
    for h in range(H):
        sq_send[:, h, :] = square
    for dk in hops[::-1]:
        k, t = other(dk, 0)
        sent.append(
            send(sq_send.at[pl.ds(k * RL, RL)], sq_recv.at[kv], sq_ss.at[dk], sq_rs.at[kv], k, t)
        )
    for i in range(4):
        c_proj[i].wait()
        total = None
        for dt in range(T):
            t = lax.rem(tp + T - dt, T)
            rows = pl.ds(pl.multiple_of(t * W, W), W)
            piece = jnp.dot(gained[dt], proj_v[i, rows, :], preferred_element_type=F32)
            total = piece if total is None else total + piece
        for h in range(H):
            part[i, :, h, :] = total[:, h * DK : (h + 1) * DK]
        for k in range(K):
            part_send[i, k] = part[i, k * RL : (k + 1) * RL].reshape(RL * H, DK).astype(BF16)
        for dk in hops[::-1]:
            k, t = other(dk, 0)
            sent.append(
                send(
                    part_send.at[i, k],
                    part_recv.at[i, kv],
                    part_ss.at[i, dk],
                    part_rs.at[i, kv],
                    k,
                    t,
                )
            )

    c_floor.wait()
    c_hgain.wait()
    square = sq_send[pl.ds(kv * RL, RL)].reshape(RL * H, DK)
    for dk in hops:
        k, t = source(dk, 0)
        arrived(sq_recv.at[k], sq_ss.at[dk], sq_rs.at[k])
        square = square + sq_recv[k].reshape(RL * H, DK)
    row_scale = lax.rsqrt(square / D + epsilon)

    def summed(i):
        total = part[i, pl.ds(kv * RL, RL)].reshape(RL * H, DK)
        for dk in hops:
            k, t = source(dk, 0)
            arrived(part_recv.at[i, k], part_ss.at[i, dk], part_rs.at[i, k])
            total = total + part_recv[i, k].astype(F32)
        return total * row_scale

    lower = sigmoid(floor_v[...])
    lower = jnp.concatenate([lower] * RL, axis=0)
    forget = lower + (1.0 - lower) * sigmoid(summed(0))
    activ = silu(summed(1))
    columns = jnp.concatenate([forget, activ], axis=0).T
    value = summed(2)
    c_past.wait()
    for s in range(RL):
        for h in range(H):
            i = s * H + h
            row = value[i : i + 1, :]
            f_col = columns[:, i : i + 1]
            q_col = columns[:, RL * H + i : RL * H + i + 1]
            new = row + f_col * (past_v[s, h] - row)
            new_v[s, h] = new
            head_v[i : i + 1, :] = jnp.sum(new * q_col, axis=0, keepdims=True)
    head_out = head_v[...]
    normed = head_out * lax.rsqrt(
        jnp.mean(head_out * head_out, axis=1, keepdims=True) + epsilon
    )
    mixed = normed * hgain_v[...] * silu(summed(3))
    mix_all[tp, kv] = mixed.astype(BF16)
    for dk, dt in near[::-1]:
        k, t = other(dk, dt)
        slot = mix_all.at[tp, kv]
        sent.append(send(slot, slot, mix_ss.at[dk, dt], mix_rs.at[kv, tp], k, t))
    c_new = pltpu.make_async_copy(new_v, new_state, local_sem.at[14])
    c_new.start()

    def spread(t, k):
        mix_f[t, pl.ds(k * RL, RL)] = mix_all[t, k].astype(F32).reshape(RL, H, DV)

    spread(tp, kv)
    for dk, dt in near:
        k, t = source(dk, dt)
        arrived(mix_all.at[t, k], mix_ss.at[dk, dt], mix_rs.at[k, t])
        spread(t, k)
    every_head = jnp.concatenate(
        [mix_f[t, :, h, :].astype(BF16) for t in range(T) for h in range(H)], axis=1
    )
    c_wout.wait()
    middle = tok_v[tp].astype(F32) + jnp.dot(
        every_head, wout_v[...], preferred_element_type=F32
    )
    middle = middle.astype(BF16)
    mid_all[me] = middle
    for dk, dt in near[::-1]:
        k, t = other(dk, dt)
        slot = mid_all.at[me]
        sent.append(send(slot, slot, mid_ss.at[dk, dt], mid_rs.at[kv, tp], k, t))

    c_mlpg.wait()
    square = jnp.zeros((R, 1), F32)
    gate = None
    if W % 128 == 0:
        groups = [[peer] for peer in [(0, 0)] + near]
    else:
        groups = [[(dk, dt) for dt in range(T)] for dk in [0] + hops]
    for group in groups:
        for dk, dt in group:
            k, t = source(dk, dt)
            if dk or dt:
                arrived(mid_all.at[k * T + t], mid_ss.at[dk, dt], mid_rs.at[k, t])
        k, t = source(*group[0])
        j = k * T + (t if len(group) == 1 else 0)
        blocks = []
        for i in range(len(group)):
            block = mid_all[j + i].astype(F32)
            square = square + jnp.sum(block * block, axis=1, keepdims=True)
            blocks.append((block * mlpg_v[j + i]).astype(BF16))
        block = jnp.concatenate(blocks, axis=1) if len(blocks) > 1 else blocks[0]
        width = len(group) * W
        lanes = pl.ds(pl.multiple_of(j * W, width), width)
        if gate is None:
            c_wgate.wait()
        g = dot_t(block, wgate_v[:, lanes])
        if gate is None:
            c_wup.wait()
        u = dot_t(block, wup_v[:, lanes])
        gate, upward = (g, u) if gate is None else (gate + g, upward + u)
    mlp_scale = lax.rsqrt(square / D + epsilon)
    hidden = (silu(gate * mlp_scale) * (upward * mlp_scale)).astype(BF16)
    c_wdown.wait()
    for dk in hops[::-1] + [0]:
        k, _ = other(dk, 0)
        lanes = pl.ds(pl.multiple_of(k * T * W, T * W), T * W)
        chunk = jnp.dot(hidden, wdown_v[:, lanes], preferred_element_type=F32).astype(BF16)
        for t in range(T):
            term_send[k * T + t] = chunk[:, t * W : (t + 1) * W]
        for dt in range(0 if dk else 1, T):
            _, t = other(dk, dt)
            sent.append(
                send(
                    term_send.at[k * T + t],
                    term_recv.at[me],
                    term_ss.at[dk, dt],
                    term_rs.at[kv, tp],
                    k,
                    t,
                )
            )
    total = term_send[me].astype(F32)
    for dk, dt in near:
        k, t = source(dk, dt)
        j = k * T + t
        arrived(term_recv.at[j], term_ss.at[dk, dt], term_rs.at[k, t])
        total = total + term_recv[j].astype(F32)
    res_v[...] = (middle.astype(F32) + total).astype(BF16)
    c_res = pltpu.make_async_copy(res_v, result, local_sem.at[15])
    c_res.start()
    for copy in sent:
        copy.wait_send()
    c_new.wait()
    c_res.wait()


def body(
    tokens,
    past_state,
    mix_gain,
    w_query,
    w_forget,
    w_value,
    w_gate_out,
    floor_logits,
    head_gain,
    w_out,
    mlp_gain,
    w_gate,
    w_up,
    w_down,
):
    K = lax.axis_size("kv")
    T = lax.axis_size("tp")
    n = K * T
    R, W = tokens.shape
    RL, H, DK, DV = past_state.shape
    args = (
        tokens,
        past_state,
        mix_gain.reshape(T, 1, W),
        w_query,
        w_forget,
        w_value,
        w_gate_out,
        floor_logits.reshape(H, DK),
        head_gain.reshape(1, DV),
        w_out,
        mlp_gain.reshape(n, 1, W),
        w_gate.T,
        w_up.T,
        w_down,
    )
    V = pltpu.VMEM
    dma = pltpu.SemaphoreType.DMA
    anywhere = pl.BlockSpec(memory_space=pl.ANY)
    return pl.pallas_call(
        functools.partial(kernel, K, T),
        out_shape=(
            jax.ShapeDtypeStruct((R, W), BF16),
            jax.ShapeDtypeStruct(past_state.shape, F32),
        ),
        in_specs=[anywhere] * len(args),
        out_specs=(anywhere, anywhere),
        scratch_shapes=[
            V((T, R, W), BF16),
            V(past_state.shape, F32),
            V((T, 1, W), F32),
            V((4,) + w_query.shape, BF16),
            V((H, DK), F32),
            V((1, DV), F32),
            V(w_out.shape, BF16),
            V((n, 1, W), F32),
            V(w_gate.shape[::-1], BF16),
            V(w_up.shape[::-1], BF16),
            V(w_down.shape, BF16),
            V(past_state.shape, F32),
            V((R, H, DK), F32),
            V((K, RL, H, DK), F32),
            V((4, R, H, DK), F32),
            V((4, K, RL * H, DK), BF16),
            V((4, K, RL * H, DK), BF16),
            V((RL * H, DV), F32),
            V((T, K, RL * H, DV), BF16),
            V((T, R, H, DV), F32),
            V((n, R, W), BF16),
            V((n, R, W), BF16),
            V((n, R, W), BF16),
            V((R, W), BF16),
            dma((16,)),
            dma((T,)),
            dma((T,)),
            dma((K,)),
            dma((K,)),
            dma((4, K)),
            dma((4, K)),
            dma((K, T)),
            dma((K, T)),
            dma((K, T)),
            dma((K, T)),
            dma((K, T)),
            dma((K, T)),
        ],
        compiler_params=pltpu.CompilerParams(
            collective_id=0, has_side_effects=True, vmem_limit_bytes=60 * 1024 * 1024
        ),
    )(*args)


def solution(mesh):
    placed = (
        P(("grp", "dp"), ("kv", "tp")),
        P(("grp", "dp", "kv"), "tp", None, None),
        P("kv"),
        P("kv", "tp"),
        P("kv", "tp"),
        P("kv", "tp"),
        P("kv", "tp"),
        P("tp"),
        P(),
        P(None, ("kv", "tp")),
        P(),
        P(None, ("kv", "tp")),
        P(None, ("kv", "tp")),
        P(("kv", "tp"), None),
    )
    return jax.shard_map(
        body,
        mesh=mesh,
        in_specs=placed,
        out_specs=(P(("grp", "dp"), ("kv", "tp")), P(("grp", "dp", "kv"), "tp", None, None)),
        check_vma=False,
    )
```

```python
import functools

import jax
import jax.numpy as jnp
from jax import lax
from jax.experimental import pallas as pl
from jax.experimental.pallas import tpu as pltpu
from jax.sharding import PartitionSpec as P

epsilon = 1e-06
F32 = jnp.float32
BF16 = jnp.bfloat16
MESH = pl.DeviceIdType.MESH


def sigmoid(a):
    return 1.0 / (1.0 + jnp.exp(-a))


def silu(a):
    return a / (1.0 + jnp.exp(-a))


def dot_t(a, b):
    return lax.dot_general(a, b, (((1,), (1,)), ((), ())), preferred_element_type=F32)


def kernel(
    K,
    T,
    tokens,
    past,
    mix_gain,
    w_query,
    w_forget,
    w_value,
    w_gate_out,
    floor_logits,
    head_gain,
    w_out,
    mlp_gain,
    w_gate,
    w_up,
    w_down,
    result,
    new_state,
    tok_v,
    past_v,
    mixg_v,
    proj_v,
    floor_v,
    hgain_v,
    wout_v,
    mlpg_v,
    wgate_v,
    wup_v,
    wdown_v,
    sq_send,
    sq_recv,
    part,
    part_send,
    part_recv,
    head_v,
    mix_all,
    mix_f,
    mid_all,
    term_send,
    term_recv,
    local_sem,
    tok_ss,
    tok_rs,
    sq_ss,
    sq_rs,
    part_ss,
    part_rs,
    mix_ss,
    mix_rs,
    mid_ss,
    mid_rs,
    term_ss,
    term_rs,
):
    R, W = tokens.shape
    RL, H, DK, DV = past.shape
    D = w_gate.shape[1]
    kv = lax.axis_index("kv")
    tp = lax.axis_index("tp")
    me = kv * T + tp

    def far(k):
        return min(k, K - k)

    hops = sorted(range(1, K), key=far)
    near = [(0, dt) for dt in range(1, T)] + [(dk, dt) for dk in hops for dt in range(T)]

    def other(dk, dt):
        return lax.rem(kv + dk, K), lax.rem(tp + dt, T)

    def source(dk, dt):
        return lax.rem(kv + K - dk, K), lax.rem(tp + T - dt, T)

    def load(i, src, dst):
        copy = pltpu.make_async_copy(src, dst, local_sem.at[i])
        copy.start()
        return copy

    c_tok = load(0, tokens, tok_v.at[tp])
    c_mixg = load(1, mix_gain, mixg_v)
    c_proj = [
        load(2 + i, w, proj_v.at[i])
        for i, w in enumerate((w_forget, w_query, w_value, w_gate_out))
    ]
    c_past = load(6, past, past_v)
    c_floor = load(7, floor_logits, floor_v)
    c_hgain = load(8, head_gain, hgain_v)
    c_mlpg = load(9, mlp_gain, mlpg_v)
    c_wout = load(10, w_out, wout_v)
    c_wgate = load(11, w_gate, wgate_v)
    c_wup = load(12, w_up, wup_v)
    c_wdown = load(13, w_down, wdown_v)

    barrier = pltpu.get_barrier_semaphore()
    for dk, dt in near:
        k, t = other(dk, dt)
        pl.semaphore_signal(barrier, inc=1, device_id={"kv": k, "tp": t}, device_id_type=MESH)
    c_tok.wait()
    pl.semaphore_wait(barrier, len(near))

    def send(src, dst, ss, rs, k, t):
        copy = pltpu.make_async_remote_copy(
            src_ref=src,
            dst_ref=dst,
            send_sem=ss,
            recv_sem=rs,
            device_id={"kv": k, "tp": t},
            device_id_type=MESH,
        )
        copy.start()
        return copy

    def arrived(dst, ss, rs):
        pltpu.make_async_remote_copy(
            src_ref=dst,
            dst_ref=dst,
            send_sem=ss,
            recv_sem=rs,
            device_id={"kv": kv, "tp": lax.rem(tp + 1, T)},
            device_id_type=MESH,
        ).wait_recv()

    sent = []
    for dt in range(1, T):
        k, t = other(0, dt)
        sent.append(send(tok_v.at[tp], tok_v.at[tp], tok_ss.at[dt], tok_rs.at[tp], k, t))

    c_mixg.wait()
    gained = []
    square = jnp.zeros((R, 1), F32)
    for dt in range(T):
        t = lax.rem(tp + T - dt, T)
        if dt:
            arrived(tok_v.at[t], tok_ss.at[0], tok_rs.at[t])
        block = tok_v[t].astype(F32)
        square = square + jnp.sum(block * block, axis=1, keepdims=True)
        gained.append((block * mixg_v[t]).astype(BF16))
    square = jnp.broadcast_to(square, (R, DK))
    for h in range(H):
        sq_send[:, h, :] = square
    for dk in hops[::-1]:
        k, t = other(dk, 0)
        sent.append(
            send(sq_send.at[pl.ds(k * RL, RL)], sq_recv.at[kv], sq_ss.at[dk], sq_rs.at[kv], k, t)
        )
    for i in range(4):
        c_proj[i].wait()
        total = None
        for dt in range(T):
            t = lax.rem(tp + T - dt, T)
            rows = pl.ds(pl.multiple_of(t * W, W), W)
            piece = jnp.dot(gained[dt], proj_v[i, rows, :], preferred_element_type=F32)
            total = piece if total is None else total + piece
        for h in range(H):
            part[i, :, h, :] = total[:, h * DK : (h + 1) * DK]
        for k in range(K):
            part_send[i, k] = part[i, k * RL : (k + 1) * RL].reshape(RL * H, DK).astype(BF16)
        for dk in hops[::-1]:
            k, t = other(dk, 0)
            sent.append(
                send(
                    part_send.at[i, k],
                    part_recv.at[i, kv],
                    part_ss.at[i, dk],
                    part_rs.at[i, kv],
                    k,
                    t,
                )
            )

    c_floor.wait()
    c_hgain.wait()
    square = sq_send[pl.ds(kv * RL, RL)].reshape(RL * H, DK)
    for dk in hops:
        k, t = source(dk, 0)
        arrived(sq_recv.at[k], sq_ss.at[dk], sq_rs.at[k])
        square = square + sq_recv[k].reshape(RL * H, DK)
    row_scale = lax.rsqrt(square / D + epsilon)

    def summed(i):
        total = part[i, pl.ds(kv * RL, RL)].reshape(RL * H, DK)
        for dk in hops:
            k, t = source(dk, 0)
            arrived(part_recv.at[i, k], part_ss.at[i, dk], part_rs.at[i, k])
            total = total + part_recv[i, k].astype(F32)
        return total * row_scale

    lower = sigmoid(floor_v[...])
    lower = jnp.concatenate([lower] * RL, axis=0)
    forget = lower + (1.0 - lower) * sigmoid(summed(0))
    activ = silu(summed(1))
    columns = jnp.concatenate([forget, activ], axis=0).T
    value = summed(2)
    c_past.wait()
    for s in range(RL):
        for h in range(H):
            i = s * H + h
            row = value[i : i + 1, :]
            f_col = columns[:, i : i + 1]
            q_col = columns[:, RL * H + i : RL * H + i + 1]
            new = row + f_col * (past_v[s, h] - row)
            new_state[s, h] = new
            head_v[i : i + 1, :] = jnp.sum(new * q_col, axis=0, keepdims=True)
    head_out = head_v[...]
    normed = head_out * lax.rsqrt(
        jnp.mean(head_out * head_out, axis=1, keepdims=True) + epsilon
    )
    mixed = normed * hgain_v[...] * silu(summed(3))
    mix_all[tp, kv] = mixed.astype(BF16)
    for dk, dt in near[::-1]:
        k, t = other(dk, dt)
        slot = mix_all.at[tp, kv]
        sent.append(send(slot, slot, mix_ss.at[dk, dt], mix_rs.at[kv, tp], k, t))

    def spread(t, k):
        mix_f[t, pl.ds(k * RL, RL)] = mix_all[t, k].astype(F32).reshape(RL, H, DV)

    spread(tp, kv)
    for dk, dt in near:
        k, t = source(dk, dt)
        arrived(mix_all.at[t, k], mix_ss.at[dk, dt], mix_rs.at[k, t])
        spread(t, k)
    every_head = jnp.concatenate(
        [mix_f[t, :, h, :].astype(BF16) for t in range(T) for h in range(H)], axis=1
    )
    c_wout.wait()
    middle = tok_v[tp].astype(F32) + jnp.dot(
        every_head, wout_v[...], preferred_element_type=F32
    )
    middle = middle.astype(BF16)
    mid_all[me] = middle
    for dk, dt in near[::-1]:
        k, t = other(dk, dt)
        slot = mid_all.at[me]
        sent.append(send(slot, slot, mid_ss.at[dk, dt], mid_rs.at[kv, tp], k, t))

    c_mlpg.wait()
    square = jnp.zeros((R, 1), F32)
    gate = None
    if W % 128 == 0:
        groups = [[peer] for peer in [(0, 0)] + near]
    else:
        groups = [[(dk, dt) for dt in range(T)] for dk in [0] + hops]
    for group in groups:
        for dk, dt in group:
            k, t = source(dk, dt)
            if dk or dt:
                arrived(mid_all.at[k * T + t], mid_ss.at[dk, dt], mid_rs.at[k, t])
        k, t = source(*group[0])
        j = k * T + (t if len(group) == 1 else 0)
        blocks = []
        for i in range(len(group)):
            block = mid_all[j + i].astype(F32)
            square = square + jnp.sum(block * block, axis=1, keepdims=True)
            blocks.append((block * mlpg_v[j + i]).astype(BF16))
        block = jnp.concatenate(blocks, axis=1) if len(blocks) > 1 else blocks[0]
        width = len(group) * W
        lanes = pl.ds(pl.multiple_of(j * W, width), width)
        if gate is None:
            c_wgate.wait()
        g = dot_t(block, wgate_v[:, lanes])
        if gate is None:
            c_wup.wait()
        u = dot_t(block, wup_v[:, lanes])
        gate, upward = (g, u) if gate is None else (gate + g, upward + u)
    mlp_scale = lax.rsqrt(square / D + epsilon)
    hidden = (silu(gate * mlp_scale) * (upward * mlp_scale)).astype(BF16)
    c_wdown.wait()
    for dk in hops[::-1] + [0]:
        k, _ = other(dk, 0)
        lanes = pl.ds(pl.multiple_of(k * T * W, T * W), T * W)
        chunk = jnp.dot(hidden, wdown_v[:, lanes], preferred_element_type=F32).astype(BF16)
        for t in range(T):
            term_send[k * T + t] = chunk[:, t * W : (t + 1) * W]
        for dt in range(0 if dk else 1, T):
            _, t = other(dk, dt)
            sent.append(
                send(
                    term_send.at[k * T + t],
                    term_recv.at[me],
                    term_ss.at[dk, dt],
                    term_rs.at[kv, tp],
                    k,
                    t,
                )
            )
    total = term_send[me].astype(F32)
    for dk, dt in near:
        k, t = source(dk, dt)
        j = k * T + t
        arrived(term_recv.at[j], term_ss.at[dk, dt], term_rs.at[k, t])
        total = total + term_recv[j].astype(F32)
    result[...] = (middle.astype(F32) + total).astype(BF16)
    for copy in sent:
        copy.wait_send()


def body(
    tokens,
    past_state,
    mix_gain,
    w_query,
    w_forget,
    w_value,
    w_gate_out,
    floor_logits,
    head_gain,
    w_out,
    mlp_gain,
    w_gate,
    w_up,
    w_down,
):
    K = lax.axis_size("kv")
    T = lax.axis_size("tp")
    n = K * T
    R, W = tokens.shape
    RL, H, DK, DV = past_state.shape
    args = (
        tokens,
        past_state,
        mix_gain.reshape(T, 1, W),
        w_query,
        w_forget,
        w_value,
        w_gate_out,
        floor_logits.reshape(H, DK),
        head_gain.reshape(1, DV),
        w_out,
        mlp_gain.reshape(n, 1, W),
        w_gate.T,
        w_up.T,
        w_down,
    )
    V = pltpu.VMEM
    dma = pltpu.SemaphoreType.DMA
    anywhere = pl.BlockSpec(memory_space=pl.ANY)
    return pl.pallas_call(
        functools.partial(kernel, K, T),
        out_shape=(
            pltpu.VMEM((R, W), BF16),
            pltpu.VMEM(past_state.shape, F32),
        ),
        in_specs=[anywhere] * len(args),
        out_specs=(pl.BlockSpec(memory_space=pltpu.VMEM),)*2,
        scratch_shapes=[
            V((T, R, W), BF16),
            V(past_state.shape, F32),
            V((T, 1, W), F32),
            V((4,) + w_query.shape, BF16),
            V((H, DK), F32),
            V((1, DV), F32),
            V(w_out.shape, BF16),
            V((n, 1, W), F32),
            V(w_gate.shape[::-1], BF16),
            V(w_up.shape[::-1], BF16),
            V(w_down.shape, BF16),
            V((R, H, DK), F32),
            V((K, RL, H, DK), F32),
            V((4, R, H, DK), F32),
            V((4, K, RL * H, DK), BF16),
            V((4, K, RL * H, DK), BF16),
            V((RL * H, DV), F32),
            V((T, K, RL * H, DV), BF16),
            V((T, R, H, DV), F32),
            V((n, R, W), BF16),
            V((n, R, W), BF16),
            V((n, R, W), BF16),
            dma((14,)),
            dma((T,)),
            dma((T,)),
            dma((K,)),
            dma((K,)),
            dma((4, K)),
            dma((4, K)),
            dma((K, T)),
            dma((K, T)),
            dma((K, T)),
            dma((K, T)),
            dma((K, T)),
            dma((K, T)),
        ],
        compiler_params=pltpu.CompilerParams(
            collective_id=0, has_side_effects=True, vmem_limit_bytes=60 * 1024 * 1024
        ),
    )(*args)


def solution(mesh):
    placed = (
        P(("grp", "dp"), ("kv", "tp")),
        P(("grp", "dp", "kv"), "tp", None, None),
        P("kv"),
        P("kv", "tp"),
        P("kv", "tp"),
        P("kv", "tp"),
        P("kv", "tp"),
        P("tp"),
        P(),
        P(None, ("kv", "tp")),
        P(),
        P(None, ("kv", "tp")),
        P(None, ("kv", "tp")),
        P(("kv", "tp"), None),
    )
    return jax.shard_map(
        body,
        mesh=mesh,
        in_specs=placed,
        out_specs=(P(("grp", "dp"), ("kv", "tp")), P(("grp", "dp", "kv"), "tp", None, None)),
        check_vma=False,
    )
```

```python
import functools

import jax
import jax.numpy as jnp
from jax import lax
from jax.experimental import pallas as pl
from jax.experimental.pallas import tpu as pltpu
from jax.sharding import PartitionSpec as P

epsilon = 1e-06
F32 = jnp.float32
BF16 = jnp.bfloat16
MESH = pl.DeviceIdType.MESH


def sigmoid(a):
    return 1.0 / (1.0 + jnp.exp(-a))


def silu(a):
    return a / (1.0 + jnp.exp(-a))


def dot_t(a, b):
    return lax.dot_general(a, b, (((1,), (1,)), ((), ())), preferred_element_type=F32)


def kernel(
    K,
    T,
    tokens,
    past,
    mix_gain,
    w_query,
    w_forget,
    w_value,
    w_gate_out,
    floor_logits,
    head_gain,
    w_out,
    mlp_gain,
    w_gate,
    w_up,
    w_down,
    result,
    new_state,
    tok_v,
    past_v,
    mixg_v,
    proj_v,
    floor_v,
    hgain_v,
    wout_v,
    mlpg_v,
    wgate_v,
    wup_v,
    wdown_v,
    sq_send,
    sq_recv,
    part,
    part_send,
    part_recv,
    head_v,
    mix_all,
    mix_f,
    mid_all,
    term_send,
    term_recv,
    local_sem,
    tok_ss,
    tok_rs,
    sq_ss,
    sq_rs,
    part_ss,
    part_rs,
    mix_ss,
    mix_rs,
    mid_ss,
    mid_rs,
    term_ss,
    term_rs,
):
    R, W = tokens.shape
    RL, H, DK, DV = past.shape
    D = w_gate.shape[1]
    kv = lax.axis_index("kv")
    tp = lax.axis_index("tp")
    me = kv * T + tp

    def far(k):
        return min(k, K - k)

    hops = sorted(range(1, K), key=far)
    near = [(0, dt) for dt in range(1, T)] + [(dk, dt) for dk in hops for dt in range(T)]

    def other(dk, dt):
        return lax.rem(kv + dk, K), lax.rem(tp + dt, T)

    def source(dk, dt):
        return lax.rem(kv + K - dk, K), lax.rem(tp + T - dt, T)

    def load(i, src, dst):
        copy = pltpu.make_async_copy(src, dst, local_sem.at[i])
        copy.start()
        return copy

    c_tok = load(0, tokens, tok_v.at[tp])
    c_mixg = load(1, mix_gain, mixg_v)
    c_proj = [
        load(2 + i, w, proj_v.at[i])
        for i, w in enumerate((w_forget, w_query, w_value, w_gate_out))
    ]
    c_past = load(6, past, past_v)
    c_floor = load(7, floor_logits, floor_v)
    c_hgain = load(8, head_gain, hgain_v)
    c_mlpg = load(9, mlp_gain, mlpg_v)
    c_wout = load(10, w_out, wout_v)
    c_wgate = load(11, w_gate, wgate_v)
    c_wup = load(12, w_up, wup_v)
    c_wdown = load(13, w_down, wdown_v)

    barrier = pltpu.get_barrier_semaphore()
    for dk, dt in near:
        k, t = other(dk, dt)
        pl.semaphore_signal(barrier, inc=1, device_id={"kv": k, "tp": t}, device_id_type=MESH)
    c_tok.wait()
    pl.semaphore_wait(barrier, len(near))

    def send(src, dst, ss, rs, k, t):
        copy = pltpu.make_async_remote_copy(
            src_ref=src,
            dst_ref=dst,
            send_sem=ss,
            recv_sem=rs,
            device_id={"kv": k, "tp": t},
            device_id_type=MESH,
        )
        copy.start()
        return copy

    def arrived(dst, ss, rs):
        pltpu.make_async_remote_copy(
            src_ref=dst,
            dst_ref=dst,
            send_sem=ss,
            recv_sem=rs,
            device_id={"kv": kv, "tp": lax.rem(tp + 1, T)},
            device_id_type=MESH,
        ).wait_recv()

    sent = []
    for dt in range(1, T):
        k, t = other(0, dt)
        sent.append(send(tok_v.at[tp], tok_v.at[tp], tok_ss.at[dt], tok_rs.at[tp], k, t))

    c_mixg.wait()
    gained = []
    early = []
    square = jnp.zeros((R, 1), F32)
    for dt in range(T):
        t = lax.rem(tp + T - dt, T)
        if dt:
            arrived(tok_v.at[t], tok_ss.at[0], tok_rs.at[t])
        block = tok_v[t].astype(F32)
        square = square + jnp.sum(block * block, axis=1, keepdims=True)
        gained.append((block * mixg_v[t]).astype(BF16))
        if dt == 0:
            rows = pl.ds(pl.multiple_of(t * W, W), W)
            for i in range(4):
                c_proj[i].wait()
                early.append(
                    jnp.dot(gained[0], proj_v[i, rows, :], preferred_element_type=F32)
                )
    square = jnp.broadcast_to(square, (R, DK))
    for h in range(H):
        sq_send[:, h, :] = square
    for dk in hops[::-1]:
        k, t = other(dk, 0)
        sent.append(
            send(sq_send.at[pl.ds(k * RL, RL)], sq_recv.at[kv], sq_ss.at[dk], sq_rs.at[kv], k, t)
        )
    for i in range(4):
        total = early[i]
        for dt in range(1, T):
            t = lax.rem(tp + T - dt, T)
            rows = pl.ds(pl.multiple_of(t * W, W), W)
            piece = jnp.dot(gained[dt], proj_v[i, rows, :], preferred_element_type=F32)
            total = total + piece
        for h in range(H):
            part[i, :, h, :] = total[:, h * DK : (h + 1) * DK]
        for k in range(K):
            part_send[i, k] = part[i, k * RL : (k + 1) * RL].reshape(RL * H, DK).astype(BF16)
        for dk in hops[::-1]:
            k, t = other(dk, 0)
            sent.append(
                send(
                    part_send.at[i, k],
                    part_recv.at[i, kv],
                    part_ss.at[i, dk],
                    part_rs.at[i, kv],
                    k,
                    t,
                )
            )

    c_floor.wait()
    c_hgain.wait()
    square = sq_send[pl.ds(kv * RL, RL)].reshape(RL * H, DK)
    for dk in hops:
        k, t = source(dk, 0)
        arrived(sq_recv.at[k], sq_ss.at[dk], sq_rs.at[k])
        square = square + sq_recv[k].reshape(RL * H, DK)
    row_scale = lax.rsqrt(square / D + epsilon)

    def summed(i):
        total = part[i, pl.ds(kv * RL, RL)].reshape(RL * H, DK)
        for dk in hops:
            k, t = source(dk, 0)
            arrived(part_recv.at[i, k], part_ss.at[i, dk], part_rs.at[i, k])
            total = total + part_recv[i, k].astype(F32)
        return total * row_scale

    lower = sigmoid(floor_v[...])
    lower = jnp.concatenate([lower] * RL, axis=0)
    forget = lower + (1.0 - lower) * sigmoid(summed(0))
    activ = silu(summed(1))
    columns = jnp.concatenate([forget, activ], axis=0).T
    value = summed(2)
    c_past.wait()
    for s in range(RL):
        for h in range(H):
            i = s * H + h
            row = value[i : i + 1, :]
            f_col = columns[:, i : i + 1]
            q_col = columns[:, RL * H + i : RL * H + i + 1]
            new = row + f_col * (past_v[s, h] - row)
            new_state[s, h] = new
            head_v[i : i + 1, :] = jnp.sum(new * q_col, axis=0, keepdims=True)
    head_out = head_v[...]
    normed = head_out * lax.rsqrt(
        jnp.mean(head_out * head_out, axis=1, keepdims=True) + epsilon
    )
    mixed = normed * hgain_v[...] * silu(summed(3))
    mix_all[tp, kv] = mixed.astype(BF16)
    for dk, dt in near[::-1]:
        k, t = other(dk, dt)
        slot = mix_all.at[tp, kv]
        sent.append(send(slot, slot, mix_ss.at[dk, dt], mix_rs.at[kv, tp], k, t))

    def spread(t, k):
        mix_f[t, pl.ds(k * RL, RL)] = mix_all[t, k].astype(F32).reshape(RL, H, DV)

    spread(tp, kv)
    for dk, dt in near:
        k, t = source(dk, dt)
        arrived(mix_all.at[t, k], mix_ss.at[dk, dt], mix_rs.at[k, t])
        spread(t, k)
    every_head = jnp.concatenate(
        [mix_f[t, :, h, :].astype(BF16) for t in range(T) for h in range(H)], axis=1
    )
    c_wout.wait()
    middle = tok_v[tp].astype(F32) + jnp.dot(
        every_head, wout_v[...], preferred_element_type=F32
    )
    middle = middle.astype(BF16)
    mid_all[me] = middle
    for dk, dt in near[::-1]:
        k, t = other(dk, dt)
        slot = mid_all.at[me]
        sent.append(send(slot, slot, mid_ss.at[dk, dt], mid_rs.at[kv, tp], k, t))

    c_mlpg.wait()
    square = jnp.zeros((R, 1), F32)
    gate = None
    if W % 128 == 0:
        groups = [[peer] for peer in [(0, 0)] + near]
    else:
        groups = [[(dk, dt) for dt in range(T)] for dk in [0] + hops]
    for group in groups:
        for dk, dt in group:
            k, t = source(dk, dt)
            if dk or dt:
                arrived(mid_all.at[k * T + t], mid_ss.at[dk, dt], mid_rs.at[k, t])
        k, t = source(*group[0])
        j = k * T + (t if len(group) == 1 else 0)
        blocks = []
        for i in range(len(group)):
            block = mid_all[j + i].astype(F32)
            square = square + jnp.sum(block * block, axis=1, keepdims=True)
            blocks.append((block * mlpg_v[j + i]).astype(BF16))
        block = jnp.concatenate(blocks, axis=1) if len(blocks) > 1 else blocks[0]
        width = len(group) * W
        lanes = pl.ds(pl.multiple_of(j * W, width), width)
        if gate is None:
            c_wgate.wait()
        g = dot_t(block, wgate_v[:, lanes])
        if gate is None:
            c_wup.wait()
        u = dot_t(block, wup_v[:, lanes])
        gate, upward = (g, u) if gate is None else (gate + g, upward + u)
    mlp_scale = lax.rsqrt(square / D + epsilon)
    hidden = (silu(gate * mlp_scale) * (upward * mlp_scale)).astype(BF16)
    c_wdown.wait()
    for dk in hops[::-1] + [0]:
        k, _ = other(dk, 0)
        lanes = pl.ds(pl.multiple_of(k * T * W, T * W), T * W)
        chunk = jnp.dot(hidden, wdown_v[:, lanes], preferred_element_type=F32).astype(BF16)
        for t in range(T):
            term_send[k * T + t] = chunk[:, t * W : (t + 1) * W]
        for dt in range(0 if dk else 1, T):
            _, t = other(dk, dt)
            sent.append(
                send(
                    term_send.at[k * T + t],
                    term_recv.at[me],
                    term_ss.at[dk, dt],
                    term_rs.at[kv, tp],
                    k,
                    t,
                )
            )
    total = term_send[me].astype(F32)
    for dk, dt in near:
        k, t = source(dk, dt)
        j = k * T + t
        arrived(term_recv.at[j], term_ss.at[dk, dt], term_rs.at[k, t])
        total = total + term_recv[j].astype(F32)
    result[...] = (middle.astype(F32) + total).astype(BF16)
    for copy in sent:
        copy.wait_send()


def body(
    tokens,
    past_state,
    mix_gain,
    w_query,
    w_forget,
    w_value,
    w_gate_out,
    floor_logits,
    head_gain,
    w_out,
    mlp_gain,
    w_gate,
    w_up,
    w_down,
):
    K = lax.axis_size("kv")
    T = lax.axis_size("tp")
    n = K * T
    R, W = tokens.shape
    RL, H, DK, DV = past_state.shape
    args = (
        tokens,
        past_state,
        mix_gain.reshape(T, 1, W),
        w_query,
        w_forget,
        w_value,
        w_gate_out,
        floor_logits.reshape(H, DK),
        head_gain.reshape(1, DV),
        w_out,
        mlp_gain.reshape(n, 1, W),
        w_gate.T,
        w_up.T,
        w_down,
    )
    V = pltpu.VMEM
    dma = pltpu.SemaphoreType.DMA
    anywhere = pl.BlockSpec(memory_space=pl.ANY)
    return pl.pallas_call(
        functools.partial(kernel, K, T),
        out_shape=(
            pltpu.VMEM((R, W), BF16),
            pltpu.VMEM(past_state.shape, F32),
        ),
        in_specs=[anywhere] * len(args),
        out_specs=(pl.BlockSpec(memory_space=pltpu.VMEM),)*2,
        scratch_shapes=[
            V((T, R, W), BF16),
            V(past_state.shape, F32),
            V((T, 1, W), F32),
            V((4,) + w_query.shape, BF16),
            V((H, DK), F32),
            V((1, DV), F32),
            V(w_out.shape, BF16),
            V((n, 1, W), F32),
            V(w_gate.shape[::-1], BF16),
            V(w_up.shape[::-1], BF16),
            V(w_down.shape, BF16),
            V((R, H, DK), F32),
            V((K, RL, H, DK), F32),
            V((4, R, H, DK), F32),
            V((4, K, RL * H, DK), BF16),
            V((4, K, RL * H, DK), BF16),
            V((RL * H, DV), F32),
            V((T, K, RL * H, DV), BF16),
            V((T, R, H, DV), F32),
            V((n, R, W), BF16),
            V((n, R, W), BF16),
            V((n, R, W), BF16),
            dma((14,)),
            dma((T,)),
            dma((T,)),
            dma((K,)),
            dma((K,)),
            dma((4, K)),
            dma((4, K)),
            dma((K, T)),
            dma((K, T)),
            dma((K, T)),
            dma((K, T)),
            dma((K, T)),
            dma((K, T)),
        ],
        compiler_params=pltpu.CompilerParams(
            collective_id=0, has_side_effects=True, vmem_limit_bytes=60 * 1024 * 1024
        ),
    )(*args)


def solution(mesh):
    placed = (
        P(("grp", "dp"), ("kv", "tp")),
        P(("grp", "dp", "kv"), "tp", None, None),
        P("kv"),
        P("kv", "tp"),
        P("kv", "tp"),
        P("kv", "tp"),
        P("kv", "tp"),
        P("tp"),
        P(),
        P(None, ("kv", "tp")),
        P(),
        P(None, ("kv", "tp")),
        P(None, ("kv", "tp")),
        P(("kv", "tp"), None),
    )
    return jax.shard_map(
        body,
        mesh=mesh,
        in_specs=placed,
        out_specs=(P(("grp", "dp"), ("kv", "tp")), P(("grp", "dp", "kv"), "tp", None, None)),
        check_vma=False,
    )
```
